128 devices in a mesh: rep: 2 (over z_hi), fs: 32 (over z_lo, y, x), tp: 2 (over core).
Axes of the slice: x: 4, y: 4, z: 4 (z_hi: 2, z_lo: 2; z = z_hi * 2 + z_lo), core: 2. Of those that a mesh axis runs over, the one named last changes fastest.
Arguments:
- resid: bfloat16 [65536, 2048], P(('rep', 'fs'), 'tp'), may hold values from -6 to 6
- gain_mix_in: float32 [2048], replicated, may hold values from 0.1 to 1.9
- u_weight: float32 [2048, 1024], P('fs', 'tp'), may hold values from -0.125 to 0.125
- v_weight: float32 [2048, 1024], P('fs', 'tp'), may hold values from -0.125 to 0.125
- u_scale: float32 [1024], P('tp'), may hold values from 0.5 to 2
- v_scale: float32 [1024], P('tp'), may hold values from 0.3 to 3
- v_gain: float32 [1024], P('tp'), may hold values from 0.1 to 1.9
- mix_matrix: float32 [16, 128, 128], P('tp'), may hold values from -0.5 to 0.5
- mix_bias: float32 [16, 128], P('tp'), may hold values from 0.1 to 1.9
- out_weight: float32 [1024, 2048], P('tp', 'fs'), may hold values from -0.1875 to 0.1875
- out_scale: float32 [2048], P('fs'), may hold values from 0.3 to 3
- gain_mix_out: float32 [2048], replicated, may hold values from 0.1 to 1.9
- gain_ffn_in: float32 [2048], replicated, may hold values from 0.1 to 1.9
- up_weight: float32 [2048, 4096], P('fs', 'tp'), may hold values from -0.125 to 0.125
- up_scale: float32 [4096], P('tp'), may hold values from 0.5 to 2
- down_weight: float32 [4096, 2048], P('tp', 'fs'), may hold values from -0.09375 to 0.09375
- down_scale: float32 [2048], P('fs'), may hold values from 0.3 to 3
- gain_ffn_out: float32 [2048], replicated, may hold values from 0.1 to 1.9
Outputs:
- result: bfloat16 [65536, 2048], P(('rep', 'fs'), 'tp')
The draws below stay inside these ranges and needn't reach their ends.
All inputs are finite; a program needn't handle non-finite values.
Results may differ from the reference program's by a relative error of at most 0.013.
Values may be sent and summed in bfloat16 or wider, within the bound.
No kernel may reach another device: no remote copies, remote signals or barrier semaphores. Data moves between devices by JAX's collectives and lax.ppermute only.
A program may use at most 128 MiB of HBM per device.

```python
import math
import jax
import jax.numpy as jnp
from jax import lax

D = 2048
A = 1024
GROUPS = 16
FF = 4096
BLOCK = 128
TOKENS = 65536
N_TP = 2


def shard_levels(key, dims, split, smallest, high):
    loudness = 1.0
    for dim, shards_of in split:
        heights = jax.random.uniform(jax.random.fold_in(jax.random.fold_in(key, 6), dim), (shards_of,), jnp.float32, smallest / len(split), high / len(split))
        loudness = loudness * jnp.repeat(jnp.exp(heights), dims[dim] // shards_of).reshape((-1,) + (1,) * (len(dims) - 1 - dim))
    return loudness


def normal_values(own_key, dims, scale, bound, shards=(), kind=jnp.bfloat16):
    loudness = shard_levels(own_key, dims, shards, -0.22, 0.18) if shards else 1.0
    drawn = jax.random.normal(own_key, dims, jnp.float32) * scale * loudness
    return jnp.minimum(jnp.maximum(drawn, -bound), bound).astype(kind)


def setup_inputs(seed: int = 0) -> dict:
    streams_of = jax.random.split(jax.random.key(seed), 19)
    return {
        "resid": normal_values(streams_of[0], (TOKENS, D), 1.0, 6.0, ((0, 64), (1, 2))),
        "gain_mix_in": jnp.clip(1.0 + 0.18 * jax.random.normal(streams_of[1], (D,), jnp.float32), 0.1, 1.9),
        "u_weight": normal_values(streams_of[2], (D, A), D ** -0.5, 0.125, ((0, 32), (1, 2)), jnp.float32),
        "v_weight": normal_values(streams_of[3], (D, A), D ** -0.5, 0.125, ((0, 32), (1, 2)), jnp.float32),
        "u_scale": jnp.clip(jnp.exp(math.log(2.0) - 1.3862944 * jax.random.uniform(streams_of[4], (A,), jnp.float32) ** shard_levels(streams_of[4], (A,), ((0, 2),), -0.2, 0.2)), 0.5, 2.0),
        "v_scale": jnp.clip(jnp.exp(math.log(3.0) - 2.3025851 * jax.random.uniform(streams_of[5], (A,), jnp.float32) ** shard_levels(streams_of[5], (A,), ((0, 2),), -0.2, 0.2)), 0.3, 3.0),
        "v_gain": jnp.clip(1.0 + 0.18 * jax.random.normal(streams_of[6], (A,), jnp.float32), 0.1, 1.9),
        "mix_matrix": normal_values(streams_of[7], (GROUPS, BLOCK, BLOCK), BLOCK ** -0.5, 0.5, ((0, 2),), jnp.float32),
        "mix_bias": jnp.clip(1.0 + 0.18 * jax.random.normal(streams_of[8], (GROUPS, BLOCK), jnp.float32), 0.1, 1.9),
        "out_weight": normal_values(streams_of[9], (A, D), A ** -0.5, 0.1875, ((0, 2), (1, 32)), jnp.float32),
        "out_scale": jnp.clip(jnp.exp(math.log(3.0) - 2.3025851 * jax.random.uniform(streams_of[10], (D,), jnp.float32) ** shard_levels(streams_of[10], (D,), ((0, 32),), -0.2, 0.2)), 0.3, 3.0),
        "gain_mix_out": jnp.clip(1.0 + 0.18 * jax.random.normal(streams_of[11], (D,), jnp.float32), 0.1, 1.9),
        "gain_ffn_in": jnp.clip(1.0 + 0.18 * jax.random.normal(streams_of[12], (D,), jnp.float32), 0.1, 1.9),
        "up_weight": normal_values(streams_of[13], (D, FF), D ** -0.5, 0.125, ((0, 32), (1, 2)), jnp.float32),
        "up_scale": jnp.clip(jnp.exp(math.log(2.0) - 1.3862944 * jax.random.uniform(streams_of[14], (FF,), jnp.float32) ** shard_levels(streams_of[14], (FF,), ((0, 2),), -0.2, 0.2)), 0.5, 2.0),
        "down_weight": normal_values(streams_of[15], (FF, D), FF ** -0.5, 0.09375, ((0, 2), (1, 32)), jnp.float32),
        "down_scale": jnp.clip(jnp.exp(math.log(3.0) - 2.3025851 * jax.random.uniform(streams_of[16], (D,), jnp.float32) ** shard_levels(streams_of[16], (D,), ((0, 32),), -0.2, 0.2)), 0.3, 3.0),
        "gain_ffn_out": jnp.clip(1.0 + 0.18 * jax.random.normal(streams_of[17], (D,), jnp.float32), 0.1, 1.9),
    }


def rms_norm(values, gain):
    power = lax.optimization_barrier(jnp.mean(values * values, axis=-1, keepdims=True))
    return values * lax.rsqrt(power + 1e-06) * gain

def split_sum(left, right, pieces):
    width = left.shape[1] // pieces
    total = jnp.zeros((left.shape[0], right.shape[1]), jnp.float32)
    for index in range(pieces):
        lower = index * width
        partial_value = jnp.dot(left[:, lower:lower + width], right[lower:lower + width], preferred_element_type=jnp.float32)
        rounded = lax.optimization_barrier(partial_value.astype(jnp.bfloat16))
        total = total + rounded.astype(jnp.float32)
    return total

def reference(resid, gain_mix_in, u_weight, v_weight, u_scale, v_scale, v_gain, mix_matrix, mix_bias, out_weight, out_scale, gain_mix_out, gain_ffn_in, up_weight, up_scale, down_weight, down_scale, gain_ffn_out):
    stream = resid.astype(jnp.float32)
    normed = rms_norm(stream, gain_mix_in).astype(jnp.bfloat16)
    u_act = jax.nn.gelu(jnp.dot(normed, u_weight.astype(jnp.bfloat16), preferred_element_type=jnp.float32) * u_scale)
    v_act = jax.nn.gelu(jnp.dot(normed, v_weight.astype(jnp.bfloat16), preferred_element_type=jnp.float32) * v_scale)
    centre = lax.optimization_barrier(jnp.mean(v_act, axis=-1, keepdims=True))
    spread = lax.optimization_barrier(jnp.mean(jnp.square(v_act - centre), axis=-1, keepdims=True))
    v_norm = ((v_act - centre) * lax.rsqrt(spread + 1e-06) * v_gain).astype(jnp.bfloat16)
    tokens = resid.shape[0]
    groups = mix_matrix.shape[0]
    blocks = v_norm.reshape(tokens // BLOCK, BLOCK, groups, A // groups).astype(jnp.float32)
    matrix = mix_matrix.astype(jnp.bfloat16).astype(jnp.float32)
    mixed = jnp.einsum('gts,bsgd->btgd', matrix, blocks) + mix_bias.T[None, :, :, None]
    gated = (u_act * mixed.reshape(tokens, A)).astype(jnp.bfloat16)
    mix_out = split_sum(gated, out_weight.astype(jnp.bfloat16), N_TP) * out_scale
    middle = (stream + rms_norm(mix_out, gain_mix_out)).astype(jnp.bfloat16)
    ffn_in = rms_norm(middle.astype(jnp.float32), gain_ffn_in).astype(jnp.bfloat16)
    raised = jnp.dot(ffn_in, up_weight.astype(jnp.bfloat16), preferred_element_type=jnp.float32) * up_scale
    hidden = jnp.square(jax.nn.relu(raised)).astype(jnp.bfloat16)
    ffn_out = split_sum(hidden, down_weight.astype(jnp.bfloat16), N_TP) * down_scale
    return (middle.astype(jnp.float32) + rms_norm(ffn_out, gain_ffn_out)).astype(jnp.bfloat16)
```

```python
import jax
import jax.numpy as jnp
from jax import lax
from jax.experimental import pallas as pl
from jax.experimental.pallas import tpu as pltpu
from jax.sharding import PartitionSpec as P

F32 = jnp.float32
BF16 = jnp.bfloat16
EPS = 1e-6
AXES = ("rep", "fs", "tp")
SIDE = 4
SHARDS = 32
ROWS = 64
HALF = SHARDS // 2

LINKS = {
    "x0": (0, 0, 1),
    "x1": (0, 0, 3),
    "y0": (0, 1, 0),
    "y1": (0, 3, 0),
    "z0": (1, 0, 0),
    "z1": (3, 0, 0),
}
ORDERS = {
    "A": ("y1", "x1", "y0", "x0", "z0"),
    "B": ("x1", "y1", "x0", "y0", "z1"),
    "C": ("y1", "y0", "x1", "z0", "x0"),
    "D": ("x1", "x0", "y1", "z1", "y0"),
    "E": ("y0", "x0", "z0", "y1", "x1"),
    "F": ("x0", "y0", "z1", "x1", "y1"),
}


def shard_mask(link):
    dz, dy, dx = LINKS[link]
    return (dz & 1) * 16 + dy * 4 + dx


def swap(array, link):
    dz, dy, dx = LINKS[link]
    pairs = []
    for z in range(SIDE):
        for y in range(SIDE):
            for x in range(SIDE):
                for core in range(2):
                    here = ((z * SIDE + y) * SIDE + x) * 2 + core
                    there = (((z ^ dz) * SIDE + (y ^ dy)) * SIDE + (x ^ dx)) * 2 + core
                    pairs.append((here, there))
    return lax.ppermute(array, AXES, pairs)


def swap_cores(array):
    return lax.ppermute(array, "tp", [(0, 1), (1, 0)])


class Stream:
    def __init__(self, piece, color):
        self.order = ORDERS[color]
        self.width = piece.shape[1]
        self.own = piece
        self.masks = [0]
        for link in self.order[:-1]:
            self.masks += [m ^ shard_mask(link) for m in self.masks]

    def run(self):
        for link in self.order[:-1]:
            self.own = jnp.concatenate([self.own, swap(self.own, link)], axis=0)
        self.got = swap(self.own, self.order[-1])
        last = shard_mask(self.order[-1])
        self.masks += [m ^ last for m in self.masks]

    @property
    def arrays(self):
        return [self.own, self.got]


def start_copies(streams, refs, whole, sems, base):
    at = 0
    for k, s in enumerate(streams):
        for j, mask in enumerate(s.masks):
            source = refs[2 * k + j // HALF]
            row = (j % HALF) * ROWS
            to = pl.multiple_of((base ^ mask) * ROWS, ROWS)
            pltpu.make_async_copy(
                source.at[pl.ds(row, ROWS), :],
                whole.at[pl.ds(to, ROWS), pl.ds(at, s.width)],
                sems.at[k],
            ).start()
        at += s.width


def wait_copies(streams, whole, sems, k):
    at = sum(s.width for s in streams[:k])
    part = whole.at[:, pl.ds(at, streams[k].width)]
    pltpu.make_async_copy(part, part, sems.at[k]).wait()


def call(body, name, grid, base, ins, streams, outs, scratch, flops):
    arrays = [a for a, _, _ in ins] + [a for s in streams for a in s.arrays]
    in_specs = [pl.BlockSpec(b, m) for _, b, m in ins]
    in_specs += [pl.BlockSpec(memory_space=pl.ANY)] * (2 * len(streams))
    return pl.pallas_call(
        body,
        name=name,
        grid_spec=pltpu.PrefetchScalarGridSpec(
            num_scalar_prefetch=1,
            grid=grid,
            in_specs=in_specs,
            out_specs=[pl.BlockSpec(b, m) for _, _, b, m in outs],
            scratch_shapes=scratch,
        ),
        out_shape=[jax.ShapeDtypeStruct(s, d) for s, d, _, _ in outs],
        cost_estimate=pl.CostEstimate(flops=flops, transcendentals=0, bytes_accessed=1 << 22),
        compiler_params=pltpu.CompilerParams(vmem_limit_bytes=40 << 20),
    )(base, *arrays)


def fixed(*_):
    return (0, 0)


def tiled(i, *_):
    return (i, 0)


def project_in(base, own, other, gain, u_scale, v_scale, streams):
    rows, part = own.shape
    tile = 256
    cols = sum(s.width for s in streams) // 2
    half = len(streams) // 2

    def body(base_ref, own_ref, other_ref, gain_ref, us_ref, vs_ref, *rest):
        refs = rest[: 2 * len(streams)]
        u_ref, v_ref, stat_ref, whole, sems = rest[2 * len(streams) :]
        first = pl.program_id(0) == 0

        @pl.when(first)
        def _():
            start_copies(streams, refs, whole, sems, base_ref[0])

        mine = own_ref[...].astype(F32)
        theirs = other_ref[...].astype(F32)
        power = jnp.sum(mine * mine, axis=1, keepdims=True) + jnp.sum(
            theirs * theirs, axis=1, keepdims=True
        )
        inverse = lax.rsqrt(power / (2 * part) + EPS)
        normed = jnp.concatenate(
            [
                (mine * inverse * gain_ref[:, :part]).astype(BF16),
                (theirs * inverse * gain_ref[:, part:]).astype(BF16),
            ],
            axis=1,
        )
        total = 0.0
        acts = []
        for k, s in enumerate(streams):

            @pl.when(first)
            def _():
                wait_copies(streams, whole, sems, k)

            at = sum(t.width for t in streams[:k])
            raised = jnp.dot(normed, whole[:, at : at + s.width], preferred_element_type=F32)
            if k < half:
                u_ref[:, at : at + s.width] = jax.nn.gelu(raised * us_ref[:, at : at + s.width])
            else:
                at -= cols
                act = jax.nn.gelu(raised * vs_ref[:, at : at + s.width])
                v_ref[:, at : at + s.width] = act
                total = total + jnp.sum(act, axis=1, keepdims=True)
                acts.append(act)
        centre = total / cols
        spread = 0.0
        for act in acts:
            spread = spread + jnp.sum(jnp.square(act - centre), axis=1, keepdims=True)
        lanes = lax.broadcasted_iota(jnp.int32, (tile, 128), 1)
        stat_ref[...] = jnp.where(lanes == 0, centre, spread)

    return call(
        body,
        "project_in",
        (rows // tile,),
        base,
        [
            (own, (tile, part), tiled),
            (other, (tile, part), tiled),
            (gain, (1, 2 * part), fixed),
            (u_scale, (1, cols), fixed),
            (v_scale, (1, cols), fixed),
        ],
        streams,
        [
            ((rows, cols), F32, (tile, cols), tiled),
            ((rows, cols), F32, (tile, cols), tiled),
            ((rows, 128), F32, (tile, 128), tiled),
        ],
        [pltpu.VMEM((2 * part, 2 * cols), BF16), pltpu.SemaphoreType.DMA((len(streams),))],
        2 * rows * 2 * part * 2 * cols,
    )


def mix_and_project(base, chunk, chunks, u_act, v_act, stats, peer_stats, v_gain, matrix, bias, streams):
    rows, cols = u_act.shape
    tile, block = 256, matrix.shape[1]
    steps = rows // chunks // tile
    width = SHARDS * ROWS
    groups = matrix.shape[0] // block
    per = cols // groups

    def body(base_ref, u_ref, v_ref, stat_ref, peer_ref, gain_ref, matrix_ref, bias_ref, *rest):
        refs = rest[: 2 * len(streams)]
        mine_ref, theirs_ref, whole, sems = rest[2 * len(streams) :]
        first = pl.program_id(0) == 0

        @pl.when(first)
        def _():
            start_copies(streams, refs, whole, sems, base_ref[0])

        mean_a, mean_b = stat_ref[:, 0:1], peer_ref[:, 0:1]
        centre = (mean_a + mean_b) * 0.5
        gap = (mean_a - mean_b) * 0.5
        spread = (stat_ref[:, 1:2] + peer_ref[:, 1:2]) / (2 * cols) + gap * gap
        v_norm = ((v_ref[...] - centre) * lax.rsqrt(spread + EPS) * gain_ref[...]).astype(BF16)
        low = lax.broadcasted_iota(jnp.int32, (block, 2 * per), 1) < per
        gated = []
        for b in range(tile // block):
            mixed = []
            for p in range(groups // 2):
                both = jnp.dot(
                    matrix_ref[2 * p * block : 2 * (p + 1) * block, :],
                    v_norm[b * block : (b + 1) * block, 2 * p * per : 2 * (p + 1) * per],
                    preferred_element_type=F32,
                )
                mixed.append(jnp.where(low, both[:block], both[block:]))
            mixed = jnp.concatenate(mixed, axis=1) + bias_ref[...]
            gated.append((u_ref[b * block : (b + 1) * block, :] * mixed).astype(BF16))
        gated = jnp.concatenate(gated, axis=0)

        @pl.when(first)
        def _():
            for k in range(len(streams)):
                wait_copies(streams, whole, sems, k)

        for ref, at in ((theirs_ref, width // 2), (mine_ref, 0)):
            ref[...] = lax.dot_general(
                gated,
                whole[at : at + width // 2, :],
                (((1,), (1,)), ((), ())),
                preferred_element_type=F32,
            ).astype(BF16)

    def shifted(i, *_):
        return (i + chunk * steps, 0)

    return call(
        body,
        f"mix_and_project_{chunk}",
        (steps,),
        base,
        [
            (u_act, (tile, cols), shifted),
            (v_act, (tile, cols), shifted),
            (stats, (tile, 128), shifted),
            (peer_stats, (tile, 128), shifted),
            (v_gain, (1, cols), fixed),
            (matrix, matrix.shape, fixed),
            (bias, bias.shape, fixed),
        ],
        streams,
        [((rows // chunks, width // 2), BF16, (tile, width // 2), tiled)] * 2,
        [pltpu.VMEM((width, cols), BF16), pltpu.SemaphoreType.DMA((len(streams),))],
        2 * rows // chunks * width * cols,
    )


def middle_of(base, chunk, chunks, sums, own, other, gain_out, gain_in):
    rows, part = own.shape
    tile = 256
    steps = rows // chunks // tile

    def body(base_ref, a_ref, b_ref, c_ref, d_ref, own_ref, other_ref, out_gain, in_gain, mid_ref, ffn_ref):
        mine = a_ref[...].astype(F32) + c_ref[...].astype(F32)
        theirs = b_ref[...].astype(F32) + d_ref[...].astype(F32)
        power = jnp.sum(mine * mine, axis=1, keepdims=True) + jnp.sum(
            theirs * theirs, axis=1, keepdims=True
        )
        inverse = lax.rsqrt(power / (2 * part) + EPS)
        mine = (own_ref[...].astype(F32) + mine * inverse * out_gain[:, :part]).astype(BF16)
        theirs = (other_ref[...].astype(F32) + theirs * inverse * out_gain[:, part:]).astype(BF16)
        mid_ref[...] = mine
        mine, theirs = mine.astype(F32), theirs.astype(F32)
        power = jnp.sum(mine * mine, axis=1, keepdims=True) + jnp.sum(
            theirs * theirs, axis=1, keepdims=True
        )
        inverse = lax.rsqrt(power / (2 * part) + EPS)
        ffn_ref[:, :part] = (mine * inverse * in_gain[:, :part]).astype(BF16)
        ffn_ref[:, part:] = (theirs * inverse * in_gain[:, part:]).astype(BF16)

    def shifted(i, *_):
        return (i + chunk * steps, 0)

    return call(
        body,
        f"middle_of_{chunk}",
        (steps,),
        base,
        [(a, (tile, part), tiled) for a in sums]
        + [
            (own, (tile, part), shifted),
            (other, (tile, part), shifted),
            (gain_out, (1, 2 * part), fixed),
            (gain_in, (1, 2 * part), fixed),
        ],
        [],
        [
            ((rows // chunks, part), BF16, (tile, part), tiled),
            ((rows // chunks, 2 * part), BF16, (tile, 2 * part), tiled),
        ],
        [],
        1 << 26,
    )


def raise_hidden(base, ffn_in, scale, streams):
    rows, width = ffn_in.shape
    tile = 256
    cols = sum(s.width for s in streams)

    def body(base_ref, x_ref, scale_ref, *rest):
        refs = rest[: 2 * len(streams)]
        out_ref, whole, sems = rest[2 * len(streams) :]
        first = pl.program_id(0) == 0

        @pl.when(first)
        def _():
            start_copies(streams, refs, whole, sems, base_ref[0])

        at = 0
        for k, s in enumerate(streams):

            @pl.when(first)
            def _():
                wait_copies(streams, whole, sems, k)

            raised = jnp.dot(x_ref[...], whole[:, at : at + s.width], preferred_element_type=F32)
            raised = jnp.maximum(raised * scale_ref[:, at : at + s.width], 0.0)
            out_ref[:, at : at + s.width] = (raised * raised).astype(BF16)
            at += s.width

    return call(
        body,
        "raise_hidden",
        (rows // tile,),
        base,
        [(ffn_in, (tile, width), tiled), (scale, (1, cols), fixed)],
        streams,
        [((rows, cols), BF16, (tile, cols), tiled)],
        [pltpu.VMEM((width, cols), BF16), pltpu.SemaphoreType.DMA((len(streams),))],
        2 * rows * width * cols,
    )[0]


def lower_hidden(base, hidden, streams):
    rows, cols = hidden.shape
    tile = 256
    width = SHARDS * ROWS

    def body(base_ref, x_ref, *rest):
        refs = rest[: 2 * len(streams)]
        mine_ref, theirs_ref, whole, sems = rest[2 * len(streams) :]

        @pl.when(pl.program_id(0) == 0)
        def _():
            start_copies(streams, refs, whole, sems, base_ref[0])
            for k in range(len(streams)):
                wait_copies(streams, whole, sems, k)

        for ref, at in ((theirs_ref, width // 2), (mine_ref, 0)):
            ref[...] = lax.dot_general(
                x_ref[...],
                whole[at : at + width // 2, :],
                (((1,), (1,)), ((), ())),
                preferred_element_type=F32,
            ).astype(BF16)

    return call(
        body,
        "lower_hidden",
        (rows // tile,),
        base,
        [(hidden, (tile, cols), tiled)],
        streams,
        [((rows, width // 2), BF16, (tile, width // 2), tiled)] * 2,
        [pltpu.VMEM((width, cols), BF16), pltpu.SemaphoreType.DMA((len(streams),))],
        2 * rows * width * cols,
    )


def cut(array, widths, colors):
    at, streams = 0, []
    for width, color in zip(widths, colors):
        streams.append(Stream(array[:, at : at + width], color))
        at += width
    return streams


def local(
    resid,
    gain_mix_in,
    u_weight,
    v_weight,
    u_scale,
    v_scale,
    v_gain,
    mix_matrix,
    mix_bias,
    out_weight,
    out_scale,
    gain_mix_out,
    gain_ffn_in,
    up_weight,
    up_scale,
    down_weight,
    down_scale,
    gain_ffn_out,
):
    rows, part = resid.shape
    lane = lax.axis_index("tp")
    base = (lax.axis_index("fs") ^ (lane * HALF)).astype(jnp.int32).reshape(1)

    def own_first(gain):
        turned = jnp.concatenate([gain[part:], gain[:part]])
        return jnp.where(lane == 0, gain, turned).reshape(1, -1)

    other = swap_cores(resid)
    u_streams = cut(u_weight.astype(BF16), (256, 256), "CD")
    v_streams = cut(v_weight.astype(BF16), (256, 256), "EF")
    in_streams = u_streams + v_streams
    out_streams = cut((out_weight * out_scale).T.astype(BF16), (512,), "A")
    up_streams = cut(up_weight.astype(BF16), (640, 640, 768), "CDB")
    down_streams = cut((down_weight * down_scale).T.astype(BF16), (768, 768, 512), "EFA")
    for s in in_streams + out_streams + up_streams + down_streams:
        s.run()

    u_act, v_act, stats = project_in(
        base,
        resid,
        other,
        own_first(gain_mix_in),
        u_scale.reshape(1, -1),
        v_scale.reshape(1, -1),
        in_streams,
    )
    peer_stats = swap_cores(stats)
    groups, block = mix_matrix.shape[:2]
    matrix = mix_matrix.astype(BF16).reshape(groups * block, block)
    bias = jnp.repeat(mix_bias.T, u_act.shape[1] // groups, axis=1)
    gain_out, gain_in = own_first(gain_mix_out), own_first(gain_ffn_in)
    chunks = 2
    middles, ffn_ins = [], []
    for chunk in range(chunks):
        mine, theirs = mix_and_project(
            base, chunk, chunks, u_act, v_act, stats, peer_stats, v_gain.reshape(1, -1), matrix, bias, out_streams
        )
        sums = [mine, theirs, swap_cores(theirs), swap_cores(mine)]
        middle, ffn_in = middle_of(base, chunk, chunks, sums, resid, other, gain_out, gain_in)
        middles.append(middle)
        ffn_ins.append(ffn_in)
    middle = jnp.concatenate(middles, axis=0)
    hidden = raise_hidden(base, jnp.concatenate(ffn_ins, axis=0), up_scale.reshape(1, -1), up_streams)
    mine, theirs = lower_hidden(base, hidden, down_streams)
    ffn_out = mine.astype(F32) + swap_cores(theirs).astype(F32)
    power = jnp.sum(ffn_out * ffn_out, axis=1)
    power = (power + swap_cores(power)).reshape(-1, 1)
    own_gain = lax.dynamic_slice_in_dim(gain_ffn_out, lane * part, part, 0)
    normed = ffn_out * lax.rsqrt(power / (2 * part) + EPS) * own_gain
    return (middle.astype(F32) + normed).astype(BF16)


def solution(mesh):
    in_specs = (
        P(("rep", "fs"), "tp"),
        P(),
        P("fs", "tp"),
        P("fs", "tp"),
        P("tp"),
        P("tp"),
        P("tp"),
        P("tp", None, None),
        P("tp", None),
        P("tp", "fs"),
        P("fs"),
        P(),
        P(),
        P("fs", "tp"),
        P("tp"),
        P("tp", "fs"),
        P("fs"),
        P(),
    )
    out_specs = P(("rep", "fs"), "tp")
    return jax.shard_map(local, mesh=mesh, in_specs=in_specs, out_specs=out_specs, check_vma=False)
```
